32 devices in a mesh: sp: 16 (over z, y, core), dp: 2 (over x).
Axes of the slice: x: 2, y: 2, z: 4, core: 2. Of those that a mesh axis runs over, the one named last changes fastest.
Arguments:
- signal: bfloat16 [2, 2048, 1024], P('dp', 'sp'), may hold values from -6 to 6
- pace: float32 [2, 16], P('dp'), may hold values from 0.5 to 2
- log_step: float32 [64], P('sp'), may hold values from -5.52 to -4.42
- a_real: float32 [64, 64], P('sp'), may hold values from -4 to -0.002, as said below
- a_imag: float32 [64, 64], P('sp'), may hold values from 0.5 to 201.06177
- in_map: float32 [64, 2, 64, 16], P('sp'), may hold values from -3 to 3
- out_map: float32 [64, 2, 16, 64], P('sp'), may hold values from -0.5 to 0.5
- skip: float32 [1024], P('sp'), may hold values from -1 to 1
- init_state: float32 [2, 2, 64, 64], P('dp', None, 'sp'), may hold values from -5 to 5
- w_glu: bfloat16 [1024, 1024], P('sp', 'dp'), may hold values from -0.1875 to 0.1875
- b_glu: float32 [1024], replicated, may hold values from -4 to 4
- g_mix: float32 [1024], replicated, may hold values from 0.1 to 1.9
- w_out: bfloat16 [1024, 4096], P('sp', 'dp'), may hold values from -0.1875 to 0.1875
Outputs:
- result: bfloat16 [2, 2048, 4096], P('dp', 'sp')
The draws below stay inside these ranges and needn't reach their ends.
Inputs may be any that keep to these rules, and one draw needn't show every extreme that they name: `a_real`: negative entries; within a group all entries are of one order.
All inputs are finite; a program needn't handle non-finite values.
Results may differ from the reference program's by a relative error of at most 0.0075.
Values may be sent and summed in bfloat16 or wider, within the bound.
A program may use at most 64 MiB of HBM per device.

```python
import math
import jax
import jax.numpy as jnp
from jax import lax

D = 4096
GROUPS = 64
C = 16
P_SIZE = 64
WIDTH = 1024
LENGTH = 2048
BATCH = 2
SPANS = 16


def draw_a_real(key, part):
    first, second, third = jax.random.split(key, 3)
    share = 0.5
    slow = jax.random.uniform(first, (GROUPS, 1), jnp.float32) < share
    slow_rate = jax.random.uniform(second, (GROUPS, P_SIZE), jnp.float32, 0.002, 0.006)
    fast_rate = jax.random.uniform(third, (GROUPS, P_SIZE), jnp.float32, 1.5, 4.0)
    return -jnp.where(slow, slow_rate, fast_rate)


def block_scale(own_key, extent, pieces, low, high):
    def one(axis_at, shards_of):
        steps = jax.random.uniform(jax.random.fold_in(jax.random.fold_in(own_key, 6), axis_at), (shards_of,), jnp.float32, low / len(pieces), high / len(pieces))
        return jnp.repeat(jnp.exp(steps), extent[axis_at] // shards_of).reshape((-1,) + (1,) * (len(extent) - axis_at - 1))

    level = one(*pieces[0])
    for cut in pieces[1:]:
        level = level * one(*cut)
    return level


def scatter_about(own_key, extent, width, reach, pieces=(), kind=jnp.bfloat16):
    factor_of = block_scale(own_key, extent, pieces, -0.22, 0.18) if pieces else 1.0
    result = jax.random.normal(own_key, extent, jnp.float32) * width * factor_of
    return jnp.minimum(jnp.maximum(result, -reach), reach).astype(kind)


def setup_inputs(seed: int = 0) -> dict:
    seeds = jax.random.split(jax.random.key(seed), 14)
    return {
        "signal": scatter_about(seeds[0], (BATCH, LENGTH, WIDTH), 1.0, 6.0, ((0, 2), (1, 16))),
        "pace": jnp.clip(jnp.exp(math.log(2.0) - 1.3862944 * jax.random.uniform(seeds[1], (BATCH, SPANS), jnp.float32) ** block_scale(seeds[1], (BATCH, SPANS), ((0, 2),), -0.2, 0.2)), 0.5, 2.0),
        "log_step": jnp.clip(-5.52 + 1.0999999 * jax.random.uniform(seeds[2], (GROUPS,), jnp.float32) ** block_scale(seeds[2], (GROUPS,), ((0, 16),), -0.2, 0.2), -5.52, -4.42),
        "a_real": draw_a_real(jax.random.fold_in(seeds[13], 71), 0),
        "a_imag": jnp.clip(0.5 + 200.56177 * jax.random.uniform(seeds[4], (GROUPS, P_SIZE), jnp.float32) ** block_scale(seeds[4], (GROUPS, P_SIZE), ((0, 16),), -0.2, 0.2), 0.5, 201.06177),
        "in_map": scatter_about(seeds[5], (GROUPS, 2, P_SIZE, C), 0.5, 3.0, ((0, 16),), jnp.float32),
        "out_map": scatter_about(seeds[6], (GROUPS, 2, C, P_SIZE), (2 * P_SIZE) ** -0.5, 0.5, ((0, 16),), jnp.float32),
        "skip": jnp.clip(jax.random.uniform(seeds[7], (WIDTH,), jnp.float32, -1.0, 1.0) * block_scale(seeds[7], (WIDTH,), ((0, 16),), -0.4, 0.0), -1.0, 1.0),
        "init_state": scatter_about(seeds[8], (BATCH, 2, GROUPS, P_SIZE), 1.0, 5.0, ((0, 2), (2, 16)), jnp.float32),
        "w_glu": scatter_about(seeds[9], (WIDTH, WIDTH), WIDTH ** -0.5, 0.1875, ((0, 16), (1, 2))),
        "b_glu": scatter_about(seeds[10], (WIDTH,), 1.0, 4.0, (), jnp.float32),
        "g_mix": jnp.clip(1.0 + 0.18 * jax.random.normal(seeds[11], (WIDTH,), jnp.float32), 0.1, 1.9),
        "w_out": scatter_about(seeds[12], (WIDTH, D), WIDTH ** -0.5, 0.1875, ((0, 16), (1, 2))),
    }


def combine(first, second):
    a1r, a1i, b1r, b1i = first
    a2r, a2i, b2r, b2i = second
    return (a2r * a1r - a2i * a1i, a2r * a1i + a2i * a1r, a2r * b1r - a2i * b1i + b2r, a2r * b1i + a2i * b1r + b2i)

def mix_group(series, pace_row, log_rate, a_re, a_im, in_map, out_map, skip_row, init):
    blocks_count = pace_row.shape[0]
    length = series.shape[0]
    span = length // blocks_count
    states = a_re.shape[0]
    steps = (jnp.exp(log_rate) * pace_row)[:, None]
    decay = jnp.exp(a_re * steps)
    bar_re = decay * jnp.cos(a_im * steps)
    bar_im = decay * jnp.sin(a_im * steps)
    modulus = a_re * a_re + a_im * a_im
    coef_re = ((bar_re - 1.0) * a_re + bar_im * a_im) / modulus
    coef_im = (bar_im * a_re - (bar_re - 1.0) * a_im) / modulus
    drive_re = coef_re[..., None] * in_map[0] - coef_im[..., None] * in_map[1]
    drive_im = coef_re[..., None] * in_map[1] + coef_im[..., None] * in_map[0]
    drive = jnp.concatenate([drive_re, drive_im], axis=1).astype(jnp.bfloat16)
    blocks = series.reshape(blocks_count, span, series.shape[1])
    inject = jnp.einsum('ksc,kpc->ksp', blocks.astype(jnp.float32), drive.astype(jnp.float32))
    inject = inject.reshape(length, 2 * states)
    in_re = inject[:, :states]
    in_im = inject[:, states:]
    in_re = in_re.at[0].add(bar_re[0] * init[0] - bar_im[0] * init[1])
    in_im = in_im.at[0].add(bar_re[0] * init[1] + bar_im[0] * init[0])
    step_re = jnp.broadcast_to(bar_re[:, None, :], (blocks_count, span, states)).reshape(length, states)
    step_im = jnp.broadcast_to(bar_im[:, None, :], (blocks_count, span, states)).reshape(length, states)
    scanned = lax.associative_scan(combine, (step_re, step_im, in_re, in_im), axis=0)
    highest = lax.Precision.HIGHEST
    response = jnp.dot(scanned[2], out_map[0].T, precision=highest) - jnp.dot(scanned[3], out_map[1].T, precision=highest)
    response = response + skip_row * series.astype(jnp.float32)
    return jax.nn.gelu(response).astype(jnp.bfloat16)

def reference(signal, pace, log_step, a_real, a_imag, in_map, out_map, skip, init_state, w_glu, b_glu, g_mix, w_out):
    grouped = signal.reshape(BATCH, LENGTH, GROUPS, C)
    skips = skip.reshape(GROUPS, C)

    def per_sequence(index):
        sample = lax.dynamic_index_in_dim(grouped, index, 0, keepdims=False)
        pace_row = lax.dynamic_index_in_dim(pace, index, 0, keepdims=False)
        init_row = lax.dynamic_index_in_dim(init_state, index, 0, keepdims=False)

        def per_group(group):
            series = lax.dynamic_index_in_dim(sample, group, 1, keepdims=False)
            start = lax.dynamic_index_in_dim(init_row, group, 1, keepdims=False)
            return mix_group(series, pace_row, log_step[group], a_real[group], a_imag[group], in_map[group], out_map[group], skips[group], start)
        outputs = lax.map(per_group, jnp.arange(GROUPS, dtype=jnp.int32))
        activated = outputs.transpose(1, 0, 2).reshape(LENGTH, WIDTH)
        gate_pre = jnp.dot(activated, w_glu, preferred_element_type=jnp.float32) + b_glu
        gated = activated.astype(jnp.float32) * jax.nn.sigmoid(gate_pre)
        scale = lax.rsqrt(lax.optimization_barrier(jnp.mean(gated * gated, axis=-1, keepdims=True)) + 1e-06)
        mixed = (gated * scale * g_mix).astype(jnp.bfloat16)
        return jnp.dot(mixed, w_out, preferred_element_type=jnp.float32).astype(jnp.bfloat16)
    return lax.map(per_sequence, jnp.arange(BATCH, dtype=jnp.int32))
```

```python
import functools
import math

import jax
import jax.numpy as jnp
from jax import lax
from jax.experimental import pallas as pl
from jax.experimental.pallas import tpu as pltpu
from jax.sharding import PartitionSpec as P

F32 = jnp.float32
BF16 = jnp.bfloat16
MESH = pl.DeviceIdType.MESH
LANES = 128
ORDERS = (("x", "y", "z"), ("y", "x", "z"), ("z", "y", "x"), ("z", "x", "y"))


def cmul(ar, ai, br, bi):
    return ar * br - ai * bi, ar * bi + ai * br


def powers(br, bi, count):
    row = lax.broadcasted_iota(jnp.int32, (8, br.shape[1]), 0)
    pr = jnp.ones((8, br.shape[1]), F32)
    pi = jnp.zeros((8, br.shape[1]), F32)
    sr, si = br, bi
    for bit in (1, 2, 4):
        qr, qi = cmul(pr, pi, sr, si)
        on = (row & bit) != 0
        pr, pi = jnp.where(on, qr, pr), jnp.where(on, qi, pi)
        sr, si = cmul(sr, si, sr, si)
    size = 8
    while size < count:
        qr, qi = cmul(pr, pi, sr, si)
        pr = jnp.concatenate([pr, qr], axis=0)
        pi = jnp.concatenate([pi, qi], axis=0)
        sr, si = cmul(sr, si, sr, si)
        size *= 2
    return pr, pi


def gelu(v):
    return 0.5 * v * (1.0 + jnp.tanh(math.sqrt(2.0 / math.pi) * (v + 0.044715 * (v * v * v))))


def kernel(
    dims, sizes,
    sig, par, pace, inm, outm, skips, b_glu, g_mix, wg_hbm, wo_hbm, out,
    buf0, buf1, buf2, buf3, tx, rx, atx, arx, bars, cmat,
    lsem, wsend, wrecv, xsend, xrecv, asend, arecv,
):
    n_sp, n_dp, tokens, wd, fold, rows, states = sizes
    bufs = (buf0, buf1, buf2, buf3)
    me = lax.axis_index("sp")
    mx = lax.axis_index("dp")
    nc, ny, nz = dims["c"], dims["y"], dims["z"]
    at = {"x": mx, "c": lax.rem(me, nc), "y": lax.rem(me // nc, ny), "z": me // (nc * ny)}
    gcols = wg_hbm.shape[1] // 4
    ocols = wo_hbm.shape[1] // 4

    def device(where):
        return {"sp": (where["z"] * ny + where["y"]) * nc + where["c"], "dp": where["x"]}

    def slot(t, where, level):
        order = ORDERS[t]
        index = [where["c"]] + [where[order[i]] for i in (2, 1, 0)][: 3 - level]
        return bufs[t].at[tuple(index)]

    local = []
    for t in range(4):
        own = slot(t, at, 0)
        local.append(pltpu.make_async_copy(
            wo_hbm.at[:, pl.ds(t * ocols, ocols)], own.at[:, pl.ds(0, ocols)], lsem.at[2 * t]))
        if gcols % LANES:
            own[:, ocols:] = wg_hbm[:, t * gcols:(t + 1) * gcols]
        else:
            local.append(pltpu.make_async_copy(
                wg_hbm.at[:, pl.ds(t * gcols, gcols)], own.at[:, pl.ds(ocols, gcols)], lsem.at[2 * t + 1]))
    for copy in local:
        copy.start()

    barrier = pltpu.get_barrier_semaphore()

    def greet(d, carry):
        pl.semaphore_signal(barrier, 1, device_id={"sp": lax.rem(me + d, n_sp), "dp": mx}, device_id_type=MESH)
        return carry

    lax.fori_loop(1, n_sp, greet, 0)
    for d in range(1, n_dp):
        pl.semaphore_signal(barrier, 1, device_id={"sp": me, "dp": lax.rem(mx + d, n_dp)}, device_id_type=MESH)

    part = lax.broadcasted_iota(jnp.int32, (rows, LANES), 1) // wd
    for tile in range(sig.shape[1] // LANES):
        pieces = [
            sig[p * rows:(p + 1) * rows, tile * LANES:(tile + 1) * LANES].astype(F32) for p in range(fold)
        ]
        for j in range(fold):
            acc = pieces[j]
            for p in range(fold):
                if p != j:
                    moved = pltpu.roll(pieces[p], ((p - j) * wd) % LANES, 1)
                    acc = jnp.where(part == p, moved, acc)
            tx[tile * fold + j] = acc.astype(BF16)

    pl.semaphore_wait(barrier, n_sp - 1 + n_dp - 1)

    def chunk_copy(src, dst, ssem, rsem, to, frm):
        return pltpu.make_async_remote_copy(
            src_ref=src, dst_ref=dst, send_sem=ssem.at[to], recv_sem=rsem.at[frm],
            device_id={"sp": to, "dp": mx}, device_id_type=MESH)

    def send_chunk(d, carry):
        to = lax.rem(me + d, n_sp)
        chunk_copy(tx.at[to], rx.at[me], xsend, xrecv, to, me).start()
        return carry

    lax.fori_loop(1, n_sp, send_chunk, 0)

    pending = []
    counter = [0]

    def post(src, where):
        k = counter[0]
        counter[0] += 1
        copy = pltpu.make_async_remote_copy(
            src_ref=src, dst_ref=src, send_sem=wsend.at[k], recv_sem=wrecv.at[k],
            device_id=device(where), device_id_type=MESH)
        copy.start()
        pending.append(copy)
        return k

    def arrive(k, dst):
        pltpu.make_async_remote_copy(
            src_ref=dst, dst_ref=dst, send_sem=wsend.at[k], recv_sem=wrecv.at[k],
            device_id=device(at), device_id_type=MESH).wait_recv()

    last = []

    def sibling(t, where, level):
        for d in range(1, nc):
            to = dict(at, c=lax.rem(at["c"] + d, nc))
            frm = dict(where, c=lax.rem(at["c"] + nc - d, nc))
            k = post(slot(t, where, level), to)
            last.append((k, slot(t, frm, level)))

    def start_stage(t, level):
        axis = ORDERS[t][level]
        n = dims[axis]
        posted = []
        ring = level == 2 and n == 4 and dims[ORDERS[t][1]] % 2 == 0
        for d in ((1, 3) if ring else range(1, n)):
            k = post(slot(t, at, level), dict(at, **{axis: lax.rem(at[axis] + d, n)}))
            posted.append((k, dict(at, **{axis: lax.rem(at[axis] + n - d, n)}), d))
        return posted

    def end_stage(t, level, posted):
        axis = ORDERS[t][level]
        n = dims[axis]
        ring = level == 2 and n == 4 and dims[ORDERS[t][1]] % 2 == 0
        halves = []
        for k, where, d in posted:
            arrive(k, slot(t, where, level))
            if ring:
                half = dims[ORDERS[t][1]] // 2
                span = pl.ds(0 if d == 1 else half, half)
                k2 = post(slot(t, where, level).at[span], dict(at, **{axis: lax.rem(at[axis] + d, n)}))
                halves.append((k2, span))
            if level > 0:
                sibling(t, where, level)
        if level == 0:
            sibling(t, at, 1)
        return halves

    def end_ring(t, halves):
        axis = ORDERS[t][2]
        where = dict(at, **{axis: lax.rem(at[axis] + 2, 4)})
        for k, span in halves:
            arrive(k, slot(t, where, 2).at[span])
        if halves:
            sibling(t, where, 2)

    for copy in local:
        copy.wait()
    stage = {t: start_stage(t, 0) for t in range(4)}

    a_re, a_im, log_step = par[0:1], par[1:2], par[2:3]
    steps = pace[...] * jnp.exp(log_step)
    real, angle = a_re * steps, a_im * steps
    decay, growth = jnp.exp(real), jnp.exp(-real)
    cos, sin = jnp.cos(angle), jnp.sin(angle)
    bar_re, bar_im = decay * cos, decay * sin
    modulus = a_re * a_re + a_im * a_im
    bars[0] = bar_re
    bars[1] = bar_im
    bars[2] = growth * cos
    bars[3] = -growth * sin
    bars[4] = ((bar_re - 1.0) * a_re + bar_im * a_im) / modulus
    bars[5] = (bar_im * a_re - (bar_re - 1.0) * a_im) / modulus
    for p in range(fold):
        for j in range(2):
            blank = [jnp.zeros((wd, states), BF16)] * fold
            blank[p] = outm[j].astype(BF16)
            cmat[2 * p + j] = jnp.concatenate(blank, axis=0)

    for t in range(4):
        end_stage(t, 0, stage[t])
        stage[t] = start_stage(t, 1)

    rx[me] = tx[me]

    def take_chunk(d, carry):
        frm = lax.rem(me + n_sp - d, n_sp)
        chunk_copy(tx.at[me], rx.at[frm], xsend, xrecv, me, frm).wait_recv()
        return carry

    lax.fori_loop(1, n_sp, take_chunk, 0)

    span_row = lax.broadcasted_iota(jnp.int32, (tokens, tokens), 0)
    span_col = lax.broadcasted_iota(jnp.int32, (tokens, tokens), 1)
    tri = jnp.where(span_row >= span_col, 1.0, 0.0).astype(BF16)
    dot = functools.partial(jnp.dot, preferred_element_type=F32)

    def dot_t(a, b):
        return lax.dot_general(a, b, (((1,), (1,)), ((), ())), preferred_element_type=F32)

    def block(k, carry):
        before_re, before_im = carry
        br, bi, gr, gi, cr, ci = [bars[j, pl.ds(k, 1), :] for j in range(6)]
        chunk = rx[k]
        drive_re = (cr * inm[0] - ci * inm[1]).astype(BF16)
        drive_im = (cr * inm[1] + ci * inm[0]).astype(BF16)
        zero = jnp.zeros_like(drive_re)

        def inject(drive):
            return jnp.concatenate(
                [dot(chunk, jnp.concatenate([drive if q == p else zero for q in range(fold)], axis=0))
                 for p in range(fold)], axis=0)

        up_re, up_im = powers(gr, gi, tokens)
        sum_re, sum_im = cmul(inject(drive_re), inject(drive_im), up_re, up_im)
        sum_re, sum_im = dot(tri, sum_re.astype(BF16)), dot(tri, sum_im.astype(BF16))
        first_re, first_im = cmul(br, bi, before_re, before_im)
        down_re, down_im = powers(br, bi, tokens)
        state_re, state_im = cmul(sum_re + first_re, sum_im + first_im, down_re, down_im)
        s_re, s_im = state_re.astype(BF16), state_im.astype(BF16)
        response = skips[...] * chunk.astype(F32)
        for p in range(fold):
            lines = slice(p * rows, (p + 1) * rows)
            response = response + dot_t(s_re[lines], cmat[2 * p]) - dot_t(s_im[lines], cmat[2 * p + 1])
        atx[k] = gelu(response).astype(BF16)

        @pl.when(k != me)
        def _():
            chunk_copy(atx.at[k], arx.at[me], asend, arecv, k, me).start()

        return state_re[tokens - 1:], state_im[tokens - 1:]

    carry = (par[3:4], par[4:5])
    cuts = [n_sp * i // 4 for i in range(5)]
    halves = {}
    for s in range(4):
        carry = lax.fori_loop(cuts[s], cuts[s + 1], block, carry)
        if s == 0:
            for t in range(4):
                end_stage(t, 1, stage[t])
                stage[t] = start_stage(t, 2)
        if s == 2:
            for t in (0, 1):
                halves[t] = end_stage(t, 2, stage[t])
    for t in (2, 3):
        halves[t] = end_stage(t, 2, stage[t])

    arx[me] = atx[me]

    def take_act(d, carry):
        frm = lax.rem(me + n_sp - d, n_sp)
        chunk_copy(atx.at[me], arx.at[frm], asend, arecv, me, frm).wait_recv()
        return carry

    lax.fori_loop(1, n_sp, take_act, 0)
    tiles = []
    for tile in range(sig.shape[1] // LANES):
        chunks = [arx[tile * fold + j].astype(F32) for j in range(fold)]
        parts = []
        for p in range(fold):
            acc = chunks[p]
            for j in range(fold):
                if j != p:
                    moved = pltpu.roll(chunks[j], ((j - p) * wd) % LANES, 1)
                    acc = jnp.where(part == j, moved, acc)
            parts.append(acc)
        tiles.append(jnp.concatenate(parts, axis=0))
    act = jnp.concatenate(tiles, axis=1)
    act_bf = act.astype(BF16)

    for t in range(4):
        end_ring(t, halves[t])
    for k, dst in last:
        arrive(k, dst)

    def weight(t, x, cols):
        order = ORDERS[t]
        found = []
        for i in range(n_sp):
            where = {"x": x, "c": i % nc, "y": (i // nc) % ny, "z": i // (nc * ny)}
            index = (where["c"],) + tuple(where[order[i2]] for i2 in (2, 1, 0))
            found.append(bufs[t][index + (slice(None), cols)])
        return jnp.concatenate(found, axis=0)

    gate = jnp.concatenate(
        [dot(act_bf, weight(t, x, slice(ocols, ocols + gcols))) for x in range(n_dp) for t in range(4)], axis=1)
    gated = act * jax.nn.sigmoid(gate + b_glu[...])
    scale = lax.rsqrt(jnp.mean(gated * gated, axis=-1, keepdims=True) + 1e-06)
    mixed = (gated * scale * g_mix[...]).astype(BF16)
    for x in range(n_dp):
        for t in range(4):
            at_col = (x * 4 + t) * ocols
            out[:, at_col:at_col + ocols] = dot(mixed, weight(t, x, slice(0, ocols))).astype(BF16)

    def drain(d, carry):
        to = lax.rem(me + d, n_sp)
        chunk_copy(tx.at[to], rx.at[me], xsend, xrecv, to, me).wait_send()
        chunk_copy(atx.at[to], arx.at[me], asend, arecv, to, me).wait_send()
        return carry

    lax.fori_loop(1, n_sp, drain, 0)
    for copy in pending:
        copy.wait_send()


def per_device(
    signal, pace, log_step, a_real, a_imag, in_map, out_map, skip, init_state, w_glu, b_glu, g_mix, w_out
):
    n_sp, n_dp = lax.axis_size("sp"), lax.axis_size("dp")
    tokens, width = signal.shape[1], signal.shape[2]
    groups, entries = a_real.shape
    channels = width // (groups * n_sp)
    wd = groups * channels
    states = groups * entries
    fold = LANES // wd
    rows = tokens // fold
    assert signal.shape[0] == 1 and pace.shape[1] == n_sp and n_sp % 4 == 0
    dims = {"x": n_dp, "c": 2, "y": 2, "z": n_sp // 4}
    eye = jnp.eye(groups, dtype=F32)
    inm = (in_map.transpose(1, 0, 3, 2)[:, :, :, None, :] * eye[None, :, None, :, None]).reshape(2, wd, states)
    outm = (out_map.transpose(1, 0, 2, 3)[:, :, :, None, :] * eye[None, :, None, :, None]).reshape(2, wd, states)
    par = jnp.stack([
        a_real.reshape(states), a_imag.reshape(states), jnp.repeat(log_step, entries),
        init_state[0, 0].reshape(states), init_state[0, 1].reshape(states)])
    pcols = (w_out.shape[1] + w_glu.shape[1]) // 4
    wrows = w_out.shape[0]
    copies = 0
    for order in ORDERS:
        n1, n2, n3 = [dims[a] for a in order]
        copies += (n1 - 1) + (n2 - 1) + (n3 - 1) + 1 + (n2 - 1) + (n3 - 1) + 4
    vmem = pl.BlockSpec(memory_space=pltpu.VMEM)
    hbm = pl.BlockSpec(memory_space=pl.ANY)
    chunk = pltpu.VMEM((n_sp, rows, LANES), BF16)
    sem = pltpu.SemaphoreType.DMA
    out_width = w_out.shape[1] * n_dp
    output = pl.pallas_call(
        functools.partial(kernel, dims, (n_sp, n_dp, tokens, wd, fold, rows, states)),
        out_shape=jax.ShapeDtypeStruct((tokens, out_width), BF16),
        in_specs=[vmem] * 8 + [vmem if w_glu.shape[1] % (4 * LANES) else hbm, hbm],
        out_specs=vmem,
        scratch_shapes=[
            pltpu.VMEM((2, dims[o[2]], dims[o[1]], dims[o[0]], wrows, pcols), BF16) for o in ORDERS
        ] + [chunk] * 4 + [
            pltpu.VMEM((6, n_sp, states), F32),
            pltpu.VMEM((2 * fold, LANES, states), BF16),
            sem((8,)), sem((copies,)), sem((copies,)),
            sem((n_sp,)), sem((n_sp,)), sem((n_sp,)), sem((n_sp,)),
        ],
        compiler_params=pltpu.CompilerParams(
            collective_id=0, has_side_effects=True, vmem_limit_bytes=56 * 1024 * 1024),
    )(
        signal[0], par, pace.reshape(n_sp, 1), inm, outm, jnp.tile(skip, fold)[None],
        b_glu[None], g_mix[None], w_glu, w_out)
    return output[None]


def solution(mesh):
    in_specs = (
        P("dp", "sp", None),
        P("dp", None),
        P("sp"),
        P("sp", None),
        P("sp", None),
        P("sp", None, None, None),
        P("sp", None, None, None),
        P("sp"),
        P("dp", None, "sp", None),
        P("sp", "dp"),
        P(),
        P(),
        P("sp", "dp"),
    )
    out_specs = P("dp", "sp", None)
    return jax.shard_map(
        per_device, mesh=mesh, in_specs=in_specs, out_specs=out_specs, check_vma=False
    )
```

```python
import functools
import math

import jax
import jax.numpy as jnp
from jax import lax
from jax.experimental import pallas as pl
from jax.experimental.pallas import tpu as pltpu
from jax.sharding import PartitionSpec as P

F32 = jnp.float32
BF16 = jnp.bfloat16
MESH = pl.DeviceIdType.MESH
LANES = 128
ORDERS = (("z", "y"), ("z", "y"), ("z", "y"), ("z", "y"), ("y", "z"))
CUTS = len(ORDERS) - 1


def cmul(ar, ai, br, bi):
    return ar * br - ai * bi, ar * bi + ai * br


def powers(br, bi, count):
    row = lax.broadcasted_iota(jnp.int32, (8, br.shape[1]), 0)
    pr = jnp.ones((8, br.shape[1]), F32)
    pi = jnp.zeros((8, br.shape[1]), F32)
    sr, si = br, bi
    for bit in (1, 2, 4):
        qr, qi = cmul(pr, pi, sr, si)
        on = (row & bit) != 0
        pr, pi = jnp.where(on, qr, pr), jnp.where(on, qi, pi)
        sr, si = cmul(sr, si, sr, si)
    size = 8
    while size < count:
        qr, qi = cmul(pr, pi, sr, si)
        pr = jnp.concatenate([pr, qr], axis=0)
        pi = jnp.concatenate([pi, qi], axis=0)
        sr, si = cmul(sr, si, sr, si)
        size *= 2
    return pr, pi


def gelu(v):
    return 0.5 * v * (1.0 + jnp.tanh(math.sqrt(2.0 / math.pi) * (v + 0.044715 * (v * v * v))))


def kernel(
    dims, sizes,
    sig, par, pace, inm, outm, skips, b_glu, g_mix, wg_hbm, wo_hbm, out,
    buf0, buf1, buf2, buf3, buf4, mrx, ostage, tx, rx, atx, arx, bars, cmat,
    lsem, wsend, wrecv, xsend, xrecv, asend, arecv, msend, mrecv, osend, orecv,
):
    n_sp, n_dp, tokens, wd, fold, rows, states = sizes
    bufs = (buf0, buf1, buf2, buf3, buf4)
    me = lax.axis_index("sp")
    mx = lax.axis_index("dp")
    nc, ny, nz = dims["c"], dims["y"], dims["z"]
    at = {"x": mx, "c": lax.rem(me, nc), "y": lax.rem(me // nc, ny), "z": me // (nc * ny)}
    gcols = wg_hbm.shape[1]
    ocols = wo_hbm.shape[1] // CUTS

    def device(where):
        return {"sp": (where["z"] * ny + where["y"]) * nc + where["c"], "dp": where["x"]}

    def slot(t, where):
        index = (where["c"], where["z"], where["y"])
        return bufs[t].at[((where["x"],) if t == 0 else ()) + index]

    local = [pltpu.make_async_copy(wg_hbm, slot(0, at), lsem.at[0])]
    for t in range(CUTS):
        local.append(pltpu.make_async_copy(
            wo_hbm.at[:, pl.ds(t * ocols, ocols)], slot(t + 1, at), lsem.at[t + 1]))
    for copy in local:
        copy.start()

    barrier = pltpu.get_barrier_semaphore()

    def greet(d, carry):
        pl.semaphore_signal(barrier, 1, device_id={"sp": lax.rem(me + d, n_sp), "dp": mx}, device_id_type=MESH)
        return carry

    lax.fori_loop(1, n_sp, greet, 0)
    for d in range(1, n_dp):
        pl.semaphore_signal(barrier, 1, device_id={"sp": me, "dp": lax.rem(mx + d, n_dp)}, device_id_type=MESH)

    part = lax.broadcasted_iota(jnp.int32, (rows, LANES), 1) // wd
    for tile in range(sig.shape[1] // LANES):
        pieces = [
            sig[p * rows:(p + 1) * rows, tile * LANES:(tile + 1) * LANES].astype(F32) for p in range(fold)
        ]
        for j in range(fold):
            acc = pieces[j]
            for p in range(fold):
                if p != j:
                    moved = pltpu.roll(pieces[p], ((p - j) * wd) % LANES, 1)
                    acc = jnp.where(part == p, moved, acc)
            tx[tile * fold + j] = acc.astype(BF16)

    pl.semaphore_wait(barrier, n_sp - 1 + n_dp - 1)

    def chunk_copy(src, dst, ssem, rsem, to, frm):
        return pltpu.make_async_remote_copy(
            src_ref=src, dst_ref=dst, send_sem=ssem.at[to], recv_sem=rsem.at[frm],
            device_id={"sp": to, "dp": mx}, device_id_type=MESH)

    def send_chunk(d, carry):
        to = lax.rem(me + d, n_sp)
        chunk_copy(tx.at[to], rx.at[me], xsend, xrecv, to, me).start()
        return carry

    lax.fori_loop(1, n_sp, send_chunk, 0)

    pending = []
    counter = [0]

    def guarded(cond, action):
        if cond is None:
            action()
        else:
            pl.when(cond)(action)

    def take():
        counter[0] += 1
        return counter[0] - 1

    def copy_of(k, ref, where):
        return pltpu.make_async_remote_copy(
            src_ref=ref, dst_ref=ref, send_sem=wsend.at[k], recv_sem=wrecv.at[k],
            device_id=device(where), device_id_type=MESH)

    def post(k, ref, where, cond=None):
        guarded(cond, lambda: copy_of(k, ref, where).start())
        pending.append((k, ref, where, cond))

    def arrive(k, ref, cond=None):
        guarded(cond, lambda: copy_of(k, ref, at).wait_recv())

    handed = {t: [] for t in range(len(ORDERS))}

    def sibling(t, where, cond):
        for d in range(1, nc):
            k = take()
            post(k, slot(t, where), dict(at, c=lax.rem(at["c"] + d, nc)), cond)
            handed[t].append((k, slot(t, dict(where, c=lax.rem(at["c"] + nc - d, nc))), cond))

    def source(move):
        where, cond = dict(at), None
        for axis, m in move.items():
            n, i = dims[axis], at[axis]
            if n == 2:
                where[axis] = 1 - i if m else i
            elif m:
                here = jnp.logical_and(i - m >= 0, i - m < n)
                cond = here if cond is None else jnp.logical_and(cond, here)
                where[axis] = jnp.clip(i - m, 0, n - 1)
        return where, cond

    def gather(t):
        order = ORDERS[t] + (("x",) if t == 0 and n_dp == 2 else ())
        wave = [(None, {axis: 0 for axis in order}, 0)]
        while wave:
            later = []
            for k, move, level in wave:
                where, cond = source(move)
                if k is not None:
                    arrive(k, slot(t, where), cond)
                for deeper in range(level, len(order)):
                    axis = order[deeper]
                    n, i, m = dims[axis], at[axis], move[axis]
                    if n == 2:
                        ways = () if m else (1,)
                    else:
                        ways = (1, -1) if m == 0 else ((m // abs(m),) if abs(m) < n - 1 else ())
                    for way in ways:
                        k2 = take()
                        if n == 2:
                            to, ok = 1 - i, cond
                        else:
                            to, ok = jnp.clip(i + way, 0, n - 1), (i < n - 1) if way == 1 else (i > 0)
                            ok = ok if cond is None else jnp.logical_and(ok, cond)
                        post(k2, slot(t, where), dict(at, **{axis: to}), ok)
                        later.append((k2, dict(move, **{axis: m + way}), deeper))
                sibling(t, where, cond)
            wave = later
            yield
        for k, ref, cond in handed[t]:
            arrive(k, ref, cond)
        if t == 0 and n_dp > 2:
            swaps = []
            for d in range(1, n_dp):
                k = take()
                post(k, bufs[0].at[mx], dict(at, x=lax.rem(mx + d, n_dp)))
                swaps.append((k, lax.rem(mx + n_dp - d, n_dp)))
            yield
            for k, frm in swaps:
                arrive(k, bufs[0].at[frm])

    runs = {t: gather(t) for t in range(len(ORDERS))}

    def advance(which=None):
        for t in range(len(ORDERS)) if which is None else (which,):
            next(runs[t], None)

    def complete(t):
        for _ in runs[t]:
            pass

    for copy in local:
        copy.wait()
    advance()

    a_re, a_im, log_step = par[0:1], par[1:2], par[2:3]
    steps = pace[...] * jnp.exp(log_step)
    real, angle = a_re * steps, a_im * steps
    decay, growth = jnp.exp(real), jnp.exp(-real)
    cos, sin = jnp.cos(angle), jnp.sin(angle)
    bar_re, bar_im = decay * cos, decay * sin
    modulus = a_re * a_re + a_im * a_im
    bars[0] = bar_re
    bars[1] = bar_im
    bars[2] = growth * cos
    bars[3] = -growth * sin
    bars[4] = ((bar_re - 1.0) * a_re + bar_im * a_im) / modulus
    bars[5] = (bar_im * a_re - (bar_re - 1.0) * a_im) / modulus
    for p in range(fold):
        for j in range(2):
            blank = [jnp.zeros((wd, states), BF16)] * fold
            blank[p] = outm[j].astype(BF16)
            cmat[2 * p + j] = jnp.concatenate(blank, axis=0)

    rx[me] = tx[me]

    def take_chunk(d, carry):
        frm = lax.rem(me + n_sp - d, n_sp)
        chunk_copy(tx.at[me], rx.at[frm], xsend, xrecv, me, frm).wait_recv()
        return carry

    lax.fori_loop(1, n_sp, take_chunk, 0)

    span_row = lax.broadcasted_iota(jnp.int32, (tokens, tokens), 0)
    span_col = lax.broadcasted_iota(jnp.int32, (tokens, tokens), 1)
    tri = jnp.where(span_row >= span_col, 1.0, 0.0).astype(BF16)
    dot = functools.partial(jnp.dot, preferred_element_type=F32)

    def dot_t(a, b):
        return lax.dot_general(a, b, (((1,), (1,)), ((), ())), preferred_element_type=F32)

    def block(k, carry):
        before_re, before_im = carry
        br, bi, gr, gi, cr, ci = [bars[j, pl.ds(k, 1), :] for j in range(6)]
        chunk = rx[k]
        drive_re = (cr * inm[0] - ci * inm[1]).astype(BF16)
        drive_im = (cr * inm[1] + ci * inm[0]).astype(BF16)
        zero = jnp.zeros_like(drive_re)

        def inject(drive):
            return jnp.concatenate(
                [dot(chunk, jnp.concatenate([drive if q == p else zero for q in range(fold)], axis=0))
                 for p in range(fold)], axis=0)

        up_re, up_im = powers(gr, gi, tokens)
        sum_re, sum_im = cmul(inject(drive_re), inject(drive_im), up_re, up_im)
        sum_re, sum_im = dot(tri, sum_re.astype(BF16)), dot(tri, sum_im.astype(BF16))
        first_re, first_im = cmul(br, bi, before_re, before_im)
        down_re, down_im = powers(br, bi, tokens)
        state_re, state_im = cmul(sum_re + first_re, sum_im + first_im, down_re, down_im)
        s_re, s_im = state_re.astype(BF16), state_im.astype(BF16)
        response = skips[...] * chunk.astype(F32)
        for p in range(fold):
            lines = slice(p * rows, (p + 1) * rows)
            response = response + dot_t(s_re[lines], cmat[2 * p]) - dot_t(s_im[lines], cmat[2 * p + 1])
        atx[k] = gelu(response).astype(BF16)

        @pl.when(k != me)
        def _():
            chunk_copy(atx.at[k], arx.at[me], asend, arecv, k, me).start()

        return state_re[tokens - 1:], state_im[tokens - 1:]

    carry = (par[3:4], par[4:5])
    advance()
    cuts = [n_sp * i // 2 for i in range(3)]
    for s in range(2):
        carry = lax.fori_loop(cuts[s], cuts[s + 1], block, carry)
        advance()

    arx[me] = atx[me]

    def take_act(d, carry):
        frm = lax.rem(me + n_sp - d, n_sp)
        chunk_copy(atx.at[me], arx.at[frm], asend, arecv, me, frm).wait_recv()
        return carry

    lax.fori_loop(1, n_sp, take_act, 0)
    tiles = []
    for tile in range(sig.shape[1] // LANES):
        chunks = [arx[tile * fold + j].astype(F32) for j in range(fold)]
        parts = []
        for p in range(fold):
            acc = chunks[p]
            for j in range(fold):
                if j != p:
                    moved = pltpu.roll(chunks[j], ((j - p) * wd) % LANES, 1)
                    acc = jnp.where(part == j, moved, acc)
            parts.append(acc)
        tiles.append(jnp.concatenate(parts, axis=0))
    act = jnp.concatenate(tiles, axis=1)
    act_bf = act.astype(BF16)

    def weight(t, x):
        found = []
        for i in range(n_sp):
            index = (i % nc, i // (nc * ny), (i // nc) % ny)
            found.append(bufs[t][((x,) if t == 0 else ()) + index])
        return jnp.concatenate(found, axis=0)

    for step in range(2 * dims["z"]):
        advance()
    complete(0)
    gate = jnp.concatenate([dot(act_bf, weight(0, x)) for x in range(n_dp)], axis=1)
    gated = act * jax.nn.sigmoid(gate + b_glu[...])
    scale = lax.rsqrt(jnp.mean(gated * gated, axis=-1, keepdims=True) + 1e-06)
    mixed = (gated * scale * g_mix[...]).astype(BF16)
    mrx[mx] = mixed

    def mixed_copy(frm, to):
        return pltpu.make_async_remote_copy(
            src_ref=mrx.at[frm], dst_ref=mrx.at[frm], send_sem=msend.at[to], recv_sem=mrecv.at[frm],
            device_id={"sp": me, "dp": to}, device_id_type=MESH)

    others = [lax.rem(mx + d, n_dp) for d in range(1, n_dp)]
    for to in others:
        mixed_copy(mx, to).start()
    for t in range(1, CUTS + 1):
        complete(t)

    def out_copy(frm, to, t):
        cols = pl.ds(pl.multiple_of((frm * CUTS + t) * ocols, LANES), ocols)
        return pltpu.make_async_remote_copy(
            src_ref=ostage.at[to, t], dst_ref=out.at[:, cols], send_sem=osend.at[to, t],
            recv_sem=orecv.at[frm, t], device_id={"sp": me, "dp": to}, device_id_type=MESH)

    for to in others:
        mixed_copy(to, mx).wait_recv()
    for t in range(CUTS):
        for to in others:
            ostage[to, t] = dot(mrx[to], weight(t + 1, None)).astype(BF16)
            out_copy(mx, to, t).start()
    for t in range(CUTS):
        cols = pl.ds(pl.multiple_of((mx * CUTS + t) * ocols, LANES), ocols)
        out[:, cols] = dot(mixed, weight(t + 1, None)).astype(BF16)
    for t in range(CUTS):
        for frm in others:
            out_copy(frm, mx, t).wait_recv()
    for to in others:
        mixed_copy(mx, to).wait_send()
        for t in range(CUTS):
            out_copy(mx, to, t).wait_send()

    def drain(d, carry):
        to = lax.rem(me + d, n_sp)
        chunk_copy(tx.at[to], rx.at[me], xsend, xrecv, to, me).wait_send()
        chunk_copy(atx.at[to], arx.at[me], asend, arecv, to, me).wait_send()
        return carry

    lax.fori_loop(1, n_sp, drain, 0)
    for k, ref, where, cond in pending:
        guarded(cond, lambda: copy_of(k, ref, where).wait_send())


def per_device(
    signal, pace, log_step, a_real, a_imag, in_map, out_map, skip, init_state, w_glu, b_glu, g_mix, w_out
):
    n_sp, n_dp = lax.axis_size("sp"), lax.axis_size("dp")
    tokens, width = signal.shape[1], signal.shape[2]
    groups, entries = a_real.shape
    channels = width // (groups * n_sp)
    wd = groups * channels
    states = groups * entries
    fold = LANES // wd
    rows = tokens // fold
    assert signal.shape[0] == 1 and pace.shape[1] == n_sp and n_sp % 4 == 0
    dims = {"x": n_dp, "c": 2, "y": 2, "z": n_sp // 4}
    eye = jnp.eye(groups, dtype=F32)
    inm = (in_map.transpose(1, 0, 3, 2)[:, :, :, None, :] * eye[None, :, None, :, None]).reshape(2, wd, states)
    outm = (out_map.transpose(1, 0, 2, 3)[:, :, :, None, :] * eye[None, :, None, :, None]).reshape(2, wd, states)
    par = jnp.stack([
        a_real.reshape(states), a_imag.reshape(states), jnp.repeat(log_step, entries),
        init_state[0, 0].reshape(states), init_state[0, 1].reshape(states)])
    wrows = w_out.shape[0]
    gcols, ocols = w_glu.shape[1], w_out.shape[1] // CUTS
    copies = 2 * (len(ORDERS) + 1) * 2 * dims["z"] * dims["y"] + n_dp
    vmem = pl.BlockSpec(memory_space=pltpu.VMEM)
    hbm = pl.BlockSpec(memory_space=pl.ANY)
    chunk = pltpu.VMEM((n_sp, rows, LANES), BF16)
    sem = pltpu.SemaphoreType.DMA
    out_width = w_out.shape[1] * n_dp
    output = pl.pallas_call(
        functools.partial(kernel, dims, (n_sp, n_dp, tokens, wd, fold, rows, states)),
        out_shape=jax.ShapeDtypeStruct((tokens, out_width), BF16),
        in_specs=[vmem] * 8 + [hbm] * 2,
        out_specs=vmem,
        scratch_shapes=[
            pltpu.VMEM(((n_dp,) if t == 0 else ()) + (2, dims["z"], dims["y"], wrows, gcols if t == 0 else ocols), BF16)
            for t in range(len(ORDERS))
        ] + [
            pltpu.VMEM((n_dp, tokens, width), BF16),
            pltpu.VMEM((n_dp, CUTS, tokens, ocols), BF16),
        ] + [chunk] * 4 + [
            pltpu.VMEM((6, n_sp, states), F32),
            pltpu.VMEM((2 * fold, LANES, states), BF16),
            sem((8,)), sem((copies,)), sem((copies,)),
            sem((n_sp,)), sem((n_sp,)), sem((n_sp,)), sem((n_sp,)),
            sem((n_dp,)), sem((n_dp,)), sem((n_dp, CUTS)), sem((n_dp, CUTS)),
        ],
        compiler_params=pltpu.CompilerParams(
            collective_id=0, has_side_effects=True, vmem_limit_bytes=56 * 1024 * 1024),
    )(
        signal[0], par, pace.reshape(n_sp, 1), inm, outm, jnp.tile(skip, fold)[None],
        b_glu[None], g_mix[None], w_glu, w_out)
    return output[None]


def solution(mesh):
    in_specs = (
        P("dp", "sp", None),
        P("dp", None),
        P("sp"),
        P("sp", None),
        P("sp", None),
        P("sp", None, None, None),
        P("sp", None, None, None),
        P("sp"),
        P("dp", None, "sp", None),
        P("sp", "dp"),
        P(),
        P(),
        P("sp", "dp"),
    )
    out_specs = P("dp", "sp", None)
    return jax.shard_map(
        per_device, mesh=mesh, in_specs=in_specs, out_specs=out_specs, check_vma=False
    )
```

```python
import functools
import math

import jax
import jax.numpy as jnp
from jax import lax
from jax.experimental import pallas as pl
from jax.experimental.pallas import tpu as pltpu
from jax.sharding import PartitionSpec as P

F32 = jnp.float32
BF16 = jnp.bfloat16
MESH = pl.DeviceIdType.MESH
LANES = 128
ORDERS = (("z", "y"),) * 5
CUTS = len(ORDERS) - 1


def spread_pieces(n_dp):
    return 2 if n_dp == 2 else 1


def cmul(ar, ai, br, bi):
    return ar * br - ai * bi, ar * bi + ai * br


def powers(br, bi, count):
    row = lax.broadcasted_iota(jnp.int32, (8, br.shape[1]), 0)
    pr = jnp.ones((8, br.shape[1]), F32)
    pi = jnp.zeros((8, br.shape[1]), F32)
    sr, si = br, bi
    for bit in (1, 2, 4):
        qr, qi = cmul(pr, pi, sr, si)
        on = (row & bit) != 0
        pr, pi = jnp.where(on, qr, pr), jnp.where(on, qi, pi)
        sr, si = cmul(sr, si, sr, si)
    size = 8
    while size < count:
        qr, qi = cmul(pr, pi, sr, si)
        pr = jnp.concatenate([pr, qr], axis=0)
        pi = jnp.concatenate([pi, qi], axis=0)
        sr, si = cmul(sr, si, sr, si)
        size *= 2
    return pr, pi


def gelu(v):
    return 0.5 * v * (1.0 + jnp.tanh(math.sqrt(2.0 / math.pi) * (v + 0.044715 * (v * v * v))))


def kernel(
    dims, sizes,
    sig, a_real, a_imag, init, in_map, out_map, log_step, pace, skip, b_glu, g_mix, wg_hbm, wo_hbm, out,
    buf0, buf1, buf2, buf3, buf4, mrx, ostage, tx, rx, atx, arx, bars, cmat,
    inm, lsem, wsend, wrecv, xsend, xrecv, asend, arecv, msend, mrecv, osend, orecv,
):
    n_sp, n_dp, tokens, wd, fold, rows, states = sizes
    spread = spread_pieces(n_dp)
    bufs = (buf0, buf1, buf2, buf3, buf4)
    me = lax.axis_index("sp")
    mx = lax.axis_index("dp")
    nc, ny, nz = dims["c"], dims["y"], dims["z"]
    at = {"x": mx, "c": lax.rem(me, nc), "y": lax.rem(me // nc, ny), "z": me // (nc * ny)}
    gcols = wg_hbm.shape[1]
    ocols = wo_hbm.shape[1] // CUTS

    def device(where):
        return {"sp": (where["z"] * ny + where["y"]) * nc + where["c"], "dp": where["x"]}

    def slot(t, where):
        index = (where["c"], where["z"], where["y"])
        return bufs[t].at[((where["x"],) if t < spread else ()) + index]

    local = [pltpu.make_async_copy(wg_hbm, slot(0, at), lsem.at[0])]
    for t in range(CUTS):
        local.append(pltpu.make_async_copy(
            wo_hbm.at[:, pl.ds(t * ocols, ocols)], slot(t + 1, at), lsem.at[t + 1]))
    for copy in local:
        copy.start()

    barrier = pltpu.get_barrier_semaphore()

    def greet(d, carry):
        pl.semaphore_signal(barrier, 1, device_id={"sp": lax.rem(me + d, n_sp), "dp": mx}, device_id_type=MESH)
        return carry

    lax.fori_loop(1, n_sp, greet, 0)
    for d in range(1, n_dp):
        pl.semaphore_signal(barrier, 1, device_id={"sp": me, "dp": lax.rem(mx + d, n_dp)}, device_id_type=MESH)

    part = lax.broadcasted_iota(jnp.int32, (rows, LANES), 1) // wd
    for tile in range(sig.shape[1] // LANES):
        pieces = [
            sig[p * rows:(p + 1) * rows, tile * LANES:(tile + 1) * LANES].astype(F32) for p in range(fold)
        ]
        for j in range(fold):
            acc = pieces[j]
            for p in range(fold):
                if p != j:
                    moved = pltpu.roll(pieces[p], ((p - j) * wd) % LANES, 1)
                    acc = jnp.where(part == p, moved, acc)
            tx[tile * fold + j] = acc.astype(BF16)

    pl.semaphore_wait(barrier, n_sp - 1 + n_dp - 1)

    def chunk_copy(src, dst, ssem, rsem, to, frm):
        return pltpu.make_async_remote_copy(
            src_ref=src, dst_ref=dst, send_sem=ssem.at[to], recv_sem=rsem.at[frm],
            device_id={"sp": to, "dp": mx}, device_id_type=MESH)

    def send_chunk(d, carry):
        to = lax.rem(me + d, n_sp)
        chunk_copy(tx.at[to], rx.at[me], xsend, xrecv, to, me).start()
        return carry

    lax.fori_loop(1, n_sp, send_chunk, 0)

    pending = []
    counter = [0]

    def guarded(cond, action):
        if cond is None:
            action()
        else:
            pl.when(cond)(action)

    def take():
        counter[0] += 1
        return counter[0] - 1

    def copy_of(k, ref, where):
        return pltpu.make_async_remote_copy(
            src_ref=ref, dst_ref=ref, send_sem=wsend.at[k], recv_sem=wrecv.at[k],
            device_id=device(where), device_id_type=MESH)

    def post(k, ref, where, cond=None):
        guarded(cond, lambda: copy_of(k, ref, where).start())
        pending.append((k, ref, where, cond))

    def arrive(k, ref, cond=None):
        guarded(cond, lambda: copy_of(k, ref, at).wait_recv())

    handed = {t: [] for t in range(len(ORDERS))}

    def sibling(t, where, cond):
        for d in range(1, nc):
            k = take()
            post(k, slot(t, where), dict(at, c=lax.rem(at["c"] + d, nc)), cond)
            handed[t].append((k, slot(t, dict(where, c=lax.rem(at["c"] + nc - d, nc))), cond))

    def source(move):
        where, cond = dict(at), None
        for axis, m in move.items():
            n, i = dims[axis], at[axis]
            if n == 2:
                where[axis] = 1 - i if m else i
            elif m:
                here = jnp.logical_and(i - m >= 0, i - m < n)
                cond = here if cond is None else jnp.logical_and(cond, here)
                where[axis] = jnp.clip(i - m, 0, n - 1)
        return where, cond

    def gather(t):
        order = ORDERS[t] + (("x",) if t < spread and n_dp == 2 else ())
        wave = [(None, {axis: 0 for axis in order}, 0)]
        while wave:
            later = []
            for k, move, level in wave:
                where, cond = source(move)
                if k is not None:
                    arrive(k, slot(t, where), cond)
                for deeper in range(level, len(order)):
                    axis = order[deeper]
                    n, i, m = dims[axis], at[axis], move[axis]
                    if n == 2:
                        ways = () if m else (1,)
                    else:
                        ways = (1, -1) if m == 0 else ((m // abs(m),) if abs(m) < n - 1 else ())
                    for way in ways:
                        k2 = take()
                        if n == 2:
                            to, ok = 1 - i, cond
                        else:
                            to, ok = jnp.clip(i + way, 0, n - 1), (i < n - 1) if way == 1 else (i > 0)
                            ok = ok if cond is None else jnp.logical_and(ok, cond)
                        post(k2, slot(t, where), dict(at, **{axis: to}), ok)
                        later.append((k2, dict(move, **{axis: m + way}), deeper))
                sibling(t, where, cond)
            wave = later
            yield
        for k, ref, cond in handed[t]:
            arrive(k, ref, cond)
        if t == 0 and n_dp > 2:
            swaps = []
            for d in range(1, n_dp):
                k = take()
                post(k, bufs[0].at[mx], dict(at, x=lax.rem(mx + d, n_dp)))
                swaps.append((k, lax.rem(mx + n_dp - d, n_dp)))
            yield
            for k, frm in swaps:
                arrive(k, bufs[0].at[frm])

    runs = {t: gather(t) for t in range(len(ORDERS))}

    def advance(which=None):
        for t in range(len(ORDERS)) if which is None else (which,):
            next(runs[t], None)

    def complete(t):
        for _ in runs[t]:
            pass

    for copy in local:
        copy.wait()
    advance()

    groups, entries = a_real.shape
    channels = wd // groups
    lane_group = lax.broadcasted_iota(jnp.int32, (1, states), 1) // entries
    block_row = lax.broadcasted_iota(jnp.int32, (n_sp, states), 0)

    def row_of(ref, *lead):
        found = [ref[lead + (slice(g, g + 1), slice(None))] for g in range(groups)]
        return jnp.concatenate(found, axis=1)

    a_re, a_im = row_of(a_real), row_of(a_imag)
    log_row = jnp.full((1, states), log_step[0], F32)
    for g in range(1, groups):
        log_row = jnp.where(lane_group == g, log_step[g], log_row)
    paces = jnp.full((n_sp, states), pace[0, 0], F32)
    for k in range(1, n_sp):
        paces = jnp.where(block_row == k, pace[0, k], paces)
    steps = paces * jnp.exp(log_row)

    def diagonal(blocks):
        lines = []
        for g in range(groups):
            line = [jnp.zeros((channels, entries), F32)] * groups
            line[g] = blocks[g]
            lines.append(jnp.concatenate(line, axis=1))
        return jnp.concatenate(lines, axis=0)

    for j in range(2):
        inm[j] = diagonal([in_map[g, j] for g in range(groups)])
    skips = jnp.concatenate([skip[...].reshape(1, wd)] * fold, axis=1)
    real, angle = a_re * steps, a_im * steps
    decay, growth = jnp.exp(real), jnp.exp(-real)
    cos, sin = jnp.cos(angle), jnp.sin(angle)
    bar_re, bar_im = decay * cos, decay * sin
    modulus = a_re * a_re + a_im * a_im
    bars[0] = bar_re
    bars[1] = bar_im
    bars[2] = growth * cos
    bars[3] = -growth * sin
    bars[4] = ((bar_re - 1.0) * a_re + bar_im * a_im) / modulus
    bars[5] = (bar_im * a_re - (bar_re - 1.0) * a_im) / modulus
    for p in range(fold):
        for j in range(2):
            blank = [jnp.zeros((wd, states), BF16)] * fold
            blank[p] = diagonal([out_map[g, j] for g in range(groups)]).astype(BF16)
            cmat[2 * p + j] = jnp.concatenate(blank, axis=0)

    rx[me] = tx[me]

    def take_chunk(d, carry):
        frm = lax.rem(me + n_sp - d, n_sp)
        chunk_copy(tx.at[me], rx.at[frm], xsend, xrecv, me, frm).wait_recv()
        return carry

    lax.fori_loop(1, n_sp, take_chunk, 0)

    span_row = lax.broadcasted_iota(jnp.int32, (tokens, tokens), 0)
    span_col = lax.broadcasted_iota(jnp.int32, (tokens, tokens), 1)
    tri = jnp.where(span_row >= span_col, 1.0, 0.0).astype(BF16)
    dot = functools.partial(jnp.dot, preferred_element_type=F32)

    def dot_t(a, b):
        return lax.dot_general(a, b, (((1,), (1,)), ((), ())), preferred_element_type=F32)

    def block(k, carry):
        before_re, before_im = carry
        br, bi, gr, gi, cr, ci = [bars[j, pl.ds(k, 1), :] for j in range(6)]
        chunk = rx[k]
        drive_re = (cr * inm[0] - ci * inm[1]).astype(BF16)
        drive_im = (cr * inm[1] + ci * inm[0]).astype(BF16)
        zero = jnp.zeros_like(drive_re)

        def inject(drive):
            return jnp.concatenate(
                [dot(chunk, jnp.concatenate([drive if q == p else zero for q in range(fold)], axis=0))
                 for p in range(fold)], axis=0)

        up_re, up_im = powers(gr, gi, tokens)
        sum_re, sum_im = cmul(inject(drive_re), inject(drive_im), up_re, up_im)
        sum_re, sum_im = dot(tri, sum_re.astype(BF16)), dot(tri, sum_im.astype(BF16))
        first_re, first_im = cmul(br, bi, before_re, before_im)
        down_re, down_im = powers(br, bi, tokens)
        state_re, state_im = cmul(sum_re + first_re, sum_im + first_im, down_re, down_im)
        s_re, s_im = state_re.astype(BF16), state_im.astype(BF16)
        response = skips * chunk.astype(F32)
        for p in range(fold):
            lines = slice(p * rows, (p + 1) * rows)
            response = response + dot_t(s_re[lines], cmat[2 * p]) - dot_t(s_im[lines], cmat[2 * p + 1])
        atx[k] = gelu(response).astype(BF16)

        @pl.when(k != me)
        def _():
            chunk_copy(atx.at[k], arx.at[me], asend, arecv, k, me).start()

        return state_re[tokens - 1:], state_im[tokens - 1:]

    carry = (row_of(init, 0, 0), row_of(init, 0, 1))
    advance()
    cuts = [n_sp * i // 2 for i in range(3)]
    for s in range(2):
        carry = lax.fori_loop(cuts[s], cuts[s + 1], block, carry)
        advance()

    arx[me] = atx[me]

    def take_act(d, carry):
        frm = lax.rem(me + n_sp - d, n_sp)
        chunk_copy(atx.at[me], arx.at[frm], asend, arecv, me, frm).wait_recv()
        return carry

    lax.fori_loop(1, n_sp, take_act, 0)
    tiles = []
    for tile in range(sig.shape[1] // LANES):
        chunks = [arx[tile * fold + j].astype(F32) for j in range(fold)]
        parts = []
        for p in range(fold):
            acc = chunks[p]
            for j in range(fold):
                if j != p:
                    moved = pltpu.roll(chunks[j], ((j - p) * wd) % LANES, 1)
                    acc = jnp.where(part == j, moved, acc)
            parts.append(acc)
        tiles.append(jnp.concatenate(parts, axis=0))
    act = jnp.concatenate(tiles, axis=1)
    act_bf = act.astype(BF16)

    def weight(t, x):
        found = []
        for i in range(n_sp):
            index = (i % nc, i // (nc * ny), (i // nc) % ny)
            found.append(bufs[t][((x,) if t < spread else ()) + index])
        return jnp.concatenate(found, axis=0)

    for step in range(2 * dims["z"]):
        advance()
    complete(0)
    gate = jnp.concatenate([dot(act_bf, weight(0, x)) for x in range(n_dp)], axis=1)
    gated = act * jax.nn.sigmoid(gate + b_glu[...].reshape(1, -1))
    scale = lax.rsqrt(jnp.mean(gated * gated, axis=-1, keepdims=True) + 1e-06)
    mixed = (gated * scale * g_mix[...].reshape(1, -1)).astype(BF16)
    mrx[mx] = mixed

    def mixed_copy(frm, to):
        return pltpu.make_async_remote_copy(
            src_ref=mrx.at[frm], dst_ref=mrx.at[frm], send_sem=msend.at[to], recv_sem=mrecv.at[frm],
            device_id={"sp": me, "dp": to}, device_id_type=MESH)

    others = [lax.rem(mx + d, n_dp) for d in range(1, n_dp)]
    for to in others:
        mixed_copy(mx, to).start()
    for t in range(1, spread):
        complete(t)
    for t in range(spread - 1):
        for x in range(n_dp):
            cols = slice((x * CUTS + t) * ocols, (x * CUTS + t + 1) * ocols)
            out[:, cols] = dot(mixed, weight(t + 1, x)).astype(BF16)
    for t in range(spread, CUTS + 1):
        complete(t)

    def out_copy(frm, to, t):
        cols = pl.ds(pl.multiple_of((frm * CUTS + t) * ocols, LANES), ocols)
        return pltpu.make_async_remote_copy(
            src_ref=ostage.at[to, t], dst_ref=out.at[:, cols], send_sem=osend.at[to, t],
            recv_sem=orecv.at[frm, t], device_id={"sp": me, "dp": to}, device_id_type=MESH)

    for to in others:
        mixed_copy(to, mx).wait_recv()
    alone = range(spread - 1, CUTS)
    for t in alone:
        for to in others:
            ostage[to, t] = dot(mrx[to], weight(t + 1, None)).astype(BF16)
            out_copy(mx, to, t).start()
    for t in alone:
        cols = pl.ds(pl.multiple_of((mx * CUTS + t) * ocols, LANES), ocols)
        out[:, cols] = dot(mixed, weight(t + 1, None)).astype(BF16)
    for t in alone:
        for frm in others:
            out_copy(frm, mx, t).wait_recv()
    for to in others:
        mixed_copy(mx, to).wait_send()
        for t in alone:
            out_copy(mx, to, t).wait_send()

    def drain(d, carry):
        to = lax.rem(me + d, n_sp)
        chunk_copy(tx.at[to], rx.at[me], xsend, xrecv, to, me).wait_send()
        chunk_copy(atx.at[to], arx.at[me], asend, arecv, to, me).wait_send()
        return carry

    lax.fori_loop(1, n_sp, drain, 0)
    for k, ref, where, cond in pending:
        guarded(cond, lambda: copy_of(k, ref, where).wait_send())


def per_device(
    signal, pace, log_step, a_real, a_imag, in_map, out_map, skip, init_state, w_glu, b_glu, g_mix, w_out
):
    n_sp, n_dp = lax.axis_size("sp"), lax.axis_size("dp")
    tokens, width = signal.shape[1], signal.shape[2]
    groups, entries = a_real.shape
    channels = width // (groups * n_sp)
    wd = groups * channels
    states = groups * entries
    fold = LANES // wd
    rows = tokens // fold
    assert signal.shape[0] == 1 and pace.shape[1] == n_sp and n_sp % 4 == 0
    dims = {"x": n_dp, "c": 2, "y": 2, "z": n_sp // 4}
    wrows = w_out.shape[0]
    gcols, ocols = w_glu.shape[1], w_out.shape[1] // CUTS
    copies = 2 * (len(ORDERS) + 3) * 2 * dims["z"] * dims["y"] + n_dp
    vmem = pl.BlockSpec(memory_space=pltpu.VMEM)
    smem = pl.BlockSpec(memory_space=pltpu.SMEM)
    hbm = pl.BlockSpec(memory_space=pl.ANY)
    chunk = pltpu.VMEM((n_sp, rows, LANES), BF16)
    sem = pltpu.SemaphoreType.DMA
    out_width = w_out.shape[1] * n_dp
    output = pl.pallas_call(
        functools.partial(kernel, dims, (n_sp, n_dp, tokens, wd, fold, rows, states)),
        out_shape=jax.ShapeDtypeStruct((tokens, out_width), BF16),
        in_specs=[vmem] * 6 + [smem] * 2 + [vmem] * 3 + [hbm] * 2,
        out_specs=vmem,
        scratch_shapes=[
            pltpu.VMEM(((n_dp,) if t < spread_pieces(n_dp) else ()) + (2, dims["z"], dims["y"], wrows, gcols if t == 0 else ocols), BF16)
            for t in range(len(ORDERS))
        ] + [
            pltpu.VMEM((n_dp, tokens, width), BF16),
            pltpu.VMEM((n_dp, CUTS, tokens, ocols), BF16),
        ] + [chunk] * 4 + [
            pltpu.VMEM((6, n_sp, states), F32),
            pltpu.VMEM((2 * fold, LANES, states), BF16),
            pltpu.VMEM((2, wd, states), F32),
            sem((8,)), sem((copies,)), sem((copies,)),
            sem((n_sp,)), sem((n_sp,)), sem((n_sp,)), sem((n_sp,)),
            sem((n_dp,)), sem((n_dp,)), sem((n_dp, CUTS)), sem((n_dp, CUTS)),
        ],
        compiler_params=pltpu.CompilerParams(
            collective_id=0, has_side_effects=True, vmem_limit_bytes=56 * 1024 * 1024),
    )(
        signal[0], a_real, a_imag, init_state, in_map.transpose(0, 1, 3, 2), out_map, log_step, pace, skip,
        b_glu, g_mix, w_glu, w_out)
    return output[None]


def solution(mesh):
    in_specs = (
        P("dp", "sp", None),
        P("dp", None),
        P("sp"),
        P("sp", None),
        P("sp", None),
        P("sp", None, None, None),
        P("sp", None, None, None),
        P("sp"),
        P("dp", None, "sp", None),
        P("sp", "dp"),
        P(),
        P(),
        P("sp", "dp"),
    )
    out_specs = P("dp", "sp", None)
    return jax.shard_map(
        per_device, mesh=mesh, in_specs=in_specs, out_specs=out_specs, check_vma=False
    )
```
